512 devices in a mesh: sp: 32 (over z, x), tp: 16 (over y, core).
Axes of the slice: x: 4, y: 8, z: 8, core: 2. Of those that a mesh axis runs over, the one named last changes fastest.
Arguments:
- stream_in: bfloat16 [8192, 2048], P(('sp', 'tp')), may hold values from -6 to 6
- queries: bfloat16 [8192, 4096], P('sp', 'tp'), may hold values from -6 to 6
- key_rows: bfloat16 [8192, 4096], P('sp', 'tp'), may hold values from -6 to 6
- values: bfloat16 [8192, 8192], P('sp', 'tp'), may hold values from -6 to 6
- decay_low: bfloat16 [8192, 16], P('sp'), may hold values from -4 to 4
- decay_matrix: bfloat16 [16, 4096], P(None, 'tp'), may hold values from -1.5 to 1.5
- decay_bias: float32 [4096], P('tp')
- decay_shift: float32 [8192, 16], P('sp', 'tp'), may hold values from -1 to 0
- head_gain: float32 [512], replicated, may hold values from 0.1 to 1.9
- output_matrix: bfloat16 [8192, 2048], P('tp'), may hold values from -0.0625 to 0.0625
- feed_gain: float32 [2048], replicated, may hold values from 0.1 to 1.9
- routes: int32 [8192, 2], P('sp'), may hold values from 0 to 31, all different within a row; in each aligned block of 256 rows (0 to 255, 256 to 511, ...) at most 16 rows name the same one
- route_weights: float32 [8192, 2], P('sp'), may hold values from 0.2 to 1
- expert_gate: bfloat16 [32, 2048, 2816], P('sp', None, 'tp'), may hold values from -0.125 to 0.125
- specialist_widen: bfloat16 [32, 2048, 2816], P('sp', None, 'tp'), may hold values from -0.125 to 0.125
- expert_down: bfloat16 [32, 2816, 2048], P('sp', 'tp'), may hold values from -0.109375 to 0.109375
Outputs:
- layer_out: bfloat16 [8192, 2048], P(('sp', 'tp'))
The draws below stay inside these ranges and needn't reach their ends.
Inputs may be any that keep to these rules, and one draw needn't show every extreme that they name: `routes`: each row names 2 different experts; within each aligned block of 256 rows no expert is named by more than 16 rows, and in every draw some expert is named by exactly 16 rows of some block.
All inputs are finite; a program needn't handle non-finite values.
Results may differ from the reference program's by a relative error of at most 0.02.
Values may be sent and summed in bfloat16 or wider, within the bound.
A program may use at most 64 MiB of HBM per device.

```python
import math
import jax
import jax.numpy as jnp
import numpy as np
from jax import lax

D = 2048
HEADS = 16
HK = 256
HV = 512
RANK = 16
FF = 2816
TOP = 2
BLK = 128
TOK_DEV = 256
SEQUENCE_LENGTH = 8192
EXPERTS = 32
CAPG = 16
N_SP = 32
N_TP = 16


def draw_decay_bias(key, part):
    key_pick = jax.random.fold_in(key, 11)
    key_slow = jax.random.fold_in(key, 12)
    key_fast = jax.random.fold_in(key, 13)
    fast_heads = jax.random.uniform(key_pick, (HEADS,), jnp.float32) < 0.5
    slow_values = jnp.log(jnp.float32(SEQUENCE_LENGTH)) + 1.0 + jax.random.uniform(key_slow, (HEADS, HK), jnp.float32, 0.0, 1.5)
    fast_values = jax.random.uniform(key_fast, (HEADS, HK), jnp.float32, -0.5, 1.0)
    return jnp.where(fast_heads[:, None], fast_values, slow_values).reshape(HEADS * HK).astype(jnp.float32)


def draw_decay_shift(key, part):
    key_rate = jax.random.fold_in(key, 21)
    key_where = jax.random.fold_in(key, 22)
    key_loss = jax.random.fold_in(key, 23)
    blocks = SEQUENCE_LENGTH // TOK_DEV
    rates = jnp.exp(jax.random.uniform(key_rate, (blocks, HEADS), jnp.float32, jnp.log(0.25), 0.0)) * (-1.5 / SEQUENCE_LENGTH)
    averaging_coefficient = jnp.repeat(rates, TOK_DEV, axis=0)
    places = jax.random.randint(key_where, (2, HEADS), 0, SEQUENCE_LENGTH)
    objective_readings = jnp.log(jax.random.uniform(key_loss, (2, HEADS), jnp.float32, 0.5, 0.8))
    positions = jnp.arange(SEQUENCE_LENGTH, dtype=jnp.int32)
    overflow_entries = (positions[:, None, None] == places[None, :, :]).astype(jnp.float32)
    cluster_batches = jnp.sum(overflow_entries * objective_readings[None, :, :], axis=1)
    return (averaging_coefficient + cluster_batches).astype(jnp.float32)


def steps_of(stream_key, shape, cuts, smallest, high):
    level = 1.0
    for dim, blocks in cuts:
        steps = jax.random.uniform(jax.random.fold_in(jax.random.fold_in(stream_key, 6), dim), (blocks,), jnp.float32, smallest / len(cuts), high / len(cuts))
        level = level * jnp.repeat(jnp.exp(steps), shape[dim] // blocks).reshape((-1,) + (1,) * (len(shape) - 1 - dim))
    return level


def assign_block(own_key, own, number, rows, amount, top, bound, skew):
    ranking = jax.random.permutation(own_key, amount)
    crowded, usual = portions_of(amount, rows * top, bound, skew, True), portions_of(amount, rows * top, bound, skew, False)
    places = jnp.arange(amount)

    def named(tallies, offset_by):
        used = int((tallies > 0).sum())
        fixed = max(1, used // 4)
        moved = fixed + (places - fixed + offset_by * (used - fixed)) % max(1, amount - fixed)
        return jnp.zeros((amount,), jnp.int32).at[ranking[jnp.where(places < fixed, places, moved)]].set(jnp.asarray(tallies, jnp.int32))

    tallies = jnp.where(number % 4 == 0, named(crowded, number // 4), named(usual, number - number // 4 - 1))
    mixed = jax.random.permutation(jax.random.fold_in(own, 3), amount)
    source_of, receiver = mixed[0:amount // 2 * 2:2], mixed[1:amount // 2 * 2:2]
    slack = jnp.minimum(tallies[source_of] - 1, bound - tallies[receiver]) // 2
    slack = jnp.where((source_of == ranking[0]) | (receiver == ranking[0]) | (tallies[receiver] == 0), 0, jnp.maximum(slack, 0))
    moved = jax.random.randint(jax.random.fold_in(own, 4), (amount // 2,), 0, 1 << 20) % (slack + 1)
    tallies = tallies.at[source_of].add(-moved).at[receiver].add(moved)
    members = jnp.searchsorted(jnp.cumsum(tallies), jnp.arange(rows * top), side="right").astype(jnp.int32)
    grid = members.reshape(top, rows).T
    grid = grid[jax.random.permutation(jax.random.fold_in(own, 1), rows)]
    offset_by = jax.random.randint(jax.random.fold_in(own, 2), (rows, 1), 0, top)
    return jnp.take_along_axis(grid, (jnp.arange(top)[None, :] + offset_by) % top, axis=1)


def portions_of(number_of, total, reach, skew, full):
    weights = [(1 << 20) // math.isqrt(rank ** skew) + 1 for rank in range(1, number_of + 1)]
    largest = reach if full else min(reach, max(-(-total // number_of), total * weights[0] // sum(weights)))
    least = 1 if total - largest >= number_of - 1 else 0
    given, surplus = [largest] + [least] * (number_of - 1), total - largest - least * (number_of - 1)
    while surplus > 0:
        free = [i for i in range(1, number_of) if given[i] < largest] or [i for i in range(1, number_of) if given[i] < reach]
        whole, remaining = sum([weights[i] for i in free]), surplus
        for i in free:
            more = min(reach - given[i], max(1, remaining * weights[i] // whole), surplus)
            given[i] = given[i] + more
            surplus = surplus - more
    return np.array(given)


def normal_values(own_key, shape, spread, most, shards=(), held_as=jnp.bfloat16):
    drawn = jax.random.normal(own_key, shape, jnp.float32) * spread
    if len(shards) > 0:
        drawn = steps_of(own_key, shape, shards, -0.22, 0.18) * drawn
    return jnp.clip(drawn, min=-most, max=most).astype(held_as)


def setup_inputs(seed: int = 0) -> dict:
    splits = jax.random.split(jax.random.key(seed), 17)
    stream_in = normal_values(splits[0], (SEQUENCE_LENGTH, D), 1.0, 6.0, ((0, 512),))
    queries = normal_values(splits[1], (SEQUENCE_LENGTH, HEADS * HK), 1.0, 6.0, ((0, 32), (1, 16)))
    key_rows = normal_values(splits[2], (SEQUENCE_LENGTH, HEADS * HK), 1.0, 6.0, ((0, 32), (1, 16)))
    values = normal_values(splits[3], (SEQUENCE_LENGTH, HEADS * HV), 1.0, 6.0, ((0, 32), (1, 16)))
    decay_low = normal_values(splits[4], (SEQUENCE_LENGTH, RANK), 1.0, 4.0, ((0, 32),))
    decay_matrix = normal_values(splits[5], (RANK, HEADS * HK), RANK ** -0.5, 1.5, ((1, 16),))
    decay_bias = draw_decay_bias(jax.random.fold_in(splits[16], 71), 0)
    decay_shift = draw_decay_shift(jax.random.fold_in(splits[16], 71), 0)
    head_gain = jnp.clip(1.0 + 0.18 * jax.random.normal(splits[8], (HV,), jnp.float32), 0.1, 1.9)
    output_matrix = normal_values(splits[9], (HEADS * HV, D), (HEADS * HV) ** -0.5, 0.0625, ((0, 16),))
    feed_gain = jnp.clip(1.0 + 0.18 * jax.random.normal(splits[10], (D,), jnp.float32), 0.1, 1.9)
    routes_keys = jax.random.split(jax.random.fold_in(splits[11], 1), SEQUENCE_LENGTH // TOK_DEV)
    routes_turns = jax.random.permutation(jax.random.fold_in(splits[11], 3), SEQUENCE_LENGTH // TOK_DEV)
    routes = jax.vmap(lambda own, number: assign_block(jax.random.fold_in(splits[11], 2), own, number, TOK_DEV, EXPERTS, TOP, CAPG, 0))(routes_keys, routes_turns).reshape((SEQUENCE_LENGTH, TOP))
    route_weights = jnp.clip(0.2 + 0.8 * jax.random.uniform(splits[12], (SEQUENCE_LENGTH, TOP), jnp.float32) ** steps_of(splits[12], (SEQUENCE_LENGTH, TOP), ((0, 32),), -0.2, 0.2), 0.2, 1.0)
    expert_gate = normal_values(splits[13], (EXPERTS, D, FF), D ** -0.5, 0.125, ((0, 32), (2, 16)))
    specialist_widen = normal_values(splits[14], (EXPERTS, D, FF), D ** -0.5, 0.125, ((0, 32), (2, 16)))
    expert_down = normal_values(splits[15], (EXPERTS, FF, D), FF ** -0.5, 0.109375, ((0, 32), (1, 16)))
    return {"stream_in": stream_in, "queries": queries, "key_rows": key_rows, "values": values, "decay_low": decay_low, "decay_matrix": decay_matrix, "decay_bias": decay_bias, "decay_shift": decay_shift, "head_gain": head_gain, "output_matrix": output_matrix, "feed_gain": feed_gain, "routes": routes, "route_weights": route_weights, "expert_gate": expert_gate, "specialist_widen": specialist_widen, "expert_down": expert_down}


TEMPER = 16.0
EPSILON = 1e-06
HIGHEST = lax.Precision.HIGHEST

def decay_logs(decay_low, decay_matrix, decay_bias, decay_shift, heads):
    before_gate = jnp.dot(decay_low, decay_matrix, preferred_element_type=jnp.float32) + decay_bias
    logged = jax.nn.log_sigmoid(before_gate) / TEMPER
    return logged.reshape(before_gate.shape[0], heads, HK) + decay_shift[:, :, None]

def into_blocks(array):
    length, heads, width = array.shape
    return array.reshape(length // BLK, BLK, heads, width).transpose(2, 0, 1, 3)

def segment_summands(queries, key_rows, values, log_decay):
    inside = jnp.cumsum(log_decay, axis=2)
    final_position = inside[:, :, -1:, :]
    scaled_query = queries * jnp.exp(inside) * HK ** (-0.5)
    scaled_key = key_rows * jnp.exp(-inside)
    end_keys = key_rows * jnp.exp(final_position - inside)
    scores = jnp.einsum('hnid,hnjd->hnij', scaled_query, scaled_key, precision=HIGHEST)
    causal = jnp.tril(jnp.ones((BLK, BLK), jnp.bool_))
    scores = jnp.where(causal, scores, 0.0)
    local_out = jnp.einsum('hnij,hnjv->hniv', scores, values, precision=HIGHEST)
    partial_update = jnp.einsum('hnjd,hnjv->hndv', end_keys, values, precision=HIGHEST)
    return (scaled_query, local_out, partial_update, jnp.exp(final_position[:, :, 0, :]))

def run_blocks(scaled_query, partial_update, block_decay, start):

    def advance(state, pieces):
        query_block, added, decay = pieces
        output = jnp.einsum('hid,hdv->hiv', query_block, state, precision=HIGHEST)
        return (state * decay[:, :, None] + added, output)
    final, outputs = lax.scan(advance, start, (jnp.moveaxis(scaled_query, 1, 0), jnp.moveaxis(partial_update, 1, 0), jnp.moveaxis(block_decay, 1, 0)))
    return (final, jnp.moveaxis(outputs, 0, 1))

def head_norm(heads_out, head_gain):
    heads = heads_out.shape[0]
    flat = heads_out.transpose(1, 2, 0, 3).reshape(-1, heads, HV)
    normed = flat * lax.rsqrt(lax.optimization_barrier(jnp.mean(flat * flat, axis=-1, keepdims=True)) + EPSILON) * head_gain
    return normed.reshape(-1, heads * HV).astype(jnp.bfloat16)

def root_scale(midstream, gain):
    return (midstream * lax.rsqrt(lax.optimization_barrier(jnp.mean(midstream * midstream, axis=-1, keepdims=True)) + EPSILON) * gain).astype(jnp.bfloat16)

def reference(stream_in, queries, key_rows, values, decay_low, decay_matrix, decay_bias, decay_shift, head_gain, output_matrix, feed_gain, routes, route_weights, expert_gate, specialist_widen, expert_down):
    log_decay = decay_logs(decay_low, decay_matrix, decay_bias, decay_shift, HEADS)

    def shaped(array, width):
        return into_blocks(array.astype(jnp.float32).reshape(SEQUENCE_LENGTH, HEADS, width))
    scaled_query, local_out, partial_update, block_decay = segment_summands(shaped(queries, HK), shaped(key_rows, HK), shaped(values, HV), into_blocks(log_decay))
    start = jnp.zeros((HEADS, HK, HV), jnp.float32)
    _, carried_out = run_blocks(scaled_query, partial_update, block_decay, start)
    mixed = head_norm(local_out + carried_out, head_gain)
    group_width = HEADS * HV // N_TP
    mixed_groups = mixed.reshape(SEQUENCE_LENGTH, N_TP, group_width).transpose(1, 0, 2)
    matrix_groups = output_matrix.reshape(N_TP, group_width, D)

    def group_step(total, inputs):
        rows_group, matrix_group = inputs
        product = jnp.dot(rows_group, matrix_group, preferred_element_type=jnp.float32)
        rounded = lax.optimization_barrier(product.astype(jnp.bfloat16))
        return (total + rounded.astype(jnp.float32), None)
    attended, _ = lax.scan(group_step, jnp.zeros((SEQUENCE_LENGTH, D), jnp.float32), (mixed_groups, matrix_groups))
    midstream = stream_in.astype(jnp.float32) + attended
    normed = root_scale(midstream, feed_gain)
    slots = N_SP * CAPG
    flat_routes = routes.reshape(-1)
    flat_weights = route_weights.reshape(-1)
    piece = FF // N_TP

    def expert_step(total, inputs):
        expert, gate_matrix, up_matrix, down_projection_weight = inputs
        matches = flat_routes == expert
        chosen = jnp.nonzero(matches, size=slots, fill_value=0)[0].astype(jnp.int32)
        live = (jnp.arange(slots, dtype=jnp.int32) < jnp.sum(matches.astype(jnp.int32))).astype(jnp.float32)
        token_index = chosen // TOP
        picked = normed[token_index]
        gated = jnp.dot(picked, gate_matrix, preferred_element_type=jnp.float32)
        lifted = jnp.dot(picked, up_matrix, preferred_element_type=jnp.float32)
        hidden = (jax.nn.silu(gated) * lifted).astype(jnp.bfloat16)
        pieces = jnp.einsum('rpf,pfd->prd', hidden.reshape(slots, N_TP, piece).astype(jnp.float32), down_projection_weight.reshape(N_TP, piece, D).astype(jnp.float32))
        rounded = lax.optimization_barrier(pieces.astype(jnp.bfloat16))
        expert_token_rows = lax.optimization_barrier(jnp.sum(rounded.astype(jnp.float32), axis=0)).astype(jnp.bfloat16)
        term = expert_token_rows.astype(jnp.float32) * (flat_weights[chosen] * live)[:, None]
        return (total.at[token_index].add(term), None)
    routed, _ = lax.scan(expert_step, jnp.zeros((SEQUENCE_LENGTH, D), jnp.float32), (jnp.arange(EXPERTS, dtype=jnp.int32), expert_gate, specialist_widen, expert_down))
    return (midstream + routed).astype(jnp.bfloat16)
```

```python
import functools

import jax
import jax.numpy as jnp
from jax import lax
from jax.experimental import pallas as pl
from jax.experimental.pallas import tpu as pltpu
from jax.sharding import PartitionSpec as P

BLK = 128
TEMPER = 16.0
EPSILON = 1e-06
PARTS = 4
BF = jnp.bfloat16
F32 = jnp.float32


def dot(a, b):
    return jnp.dot(a, b, preferred_element_type=F32)


def dot_nt(a, b):
    return lax.dot_general(a, b, (((1,), (1,)), ((), ())), preferred_element_type=F32)


def split2(x):
    high = x.astype(BF)
    return high, (x - high.astype(F32)).astype(BF)


def split3(x):
    high = x.astype(BF)
    rest = x - high.astype(F32)
    middle = rest.astype(BF)
    return high, middle, (rest - middle.astype(F32)).astype(BF)


def remote(src, dst, send_sem, recv_sem, device):
    return pltpu.make_async_remote_copy(
        src_ref=src,
        dst_ref=dst,
        send_sem=send_sem,
        recv_sem=recv_sem,
        device_id=device,
        device_id_type=pl.DeviceIdType.MESH,
    )


def iota(shape, dim):
    return lax.broadcasted_iota(jnp.int32, shape, dim)


def layer_kernel(
    size,
    stream,
    queries,
    key_rows,
    values,
    decay_low,
    decay_matrix,
    decay_bias,
    decay_shift,
    head_gain,
    w_any,
    feed_gain,
    routes,
    route_weights,
    gate_any,
    up_any,
    down_any,
    out,
    w_s,
    gate_s,
    up_s,
    down_s,
    query_s,
    total_s,
    update_s,
    state_send,
    state_recv,
    prior_send,
    prior_recv,
    select_s,
    weight_high,
    weight_low,
    mixed_s,
    pair_send,
    pair_recv,
    own_s,
    row_send,
    row_recv,
    mid_s,
    norm_send,
    norm_recv,
    slot_send,
    rows_s,
    gate_acc,
    up_acc,
    hidden_s,
    half_send,
    half_recv,
    half_own,
    sum_send,
    sum_recv,
    back_send,
    back_recv,
    last_send,
    last_recv,
    load_sem,
    state_ss,
    state_rs,
    prior_ss,
    prior_rs,
    pair_ss,
    pair_rs,
    row_ss,
    row_rs,
    norm_ss,
    norm_rs,
    slot_ss,
    slot_rs,
    ring_ss,
    ring_rs,
    mate_ss,
    mate_rs,
    half_ss,
    half_rs,
    sum_ss,
    sum_rs,
    back_ss,
    back_rs,
    last_ss,
    last_rs,
):
    n_sp, n_tp, rows, width, piece = size
    n_y = n_tp // 2
    half_ring = n_y // 2
    length = rows * n_tp
    slots = 2 * length // n_sp
    columns = width // n_tp
    part_width = width // PARTS
    hk = queries.shape[1]
    hv = values.shape[1]
    sp = lax.axis_index("sp")
    tp = lax.axis_index("tp")
    y = lax.div(tp, 2)
    core = lax.rem(tp, 2)
    other = 1 - core
    mate = (sp, tp + 1 - 2 * core)

    loads = []
    for i, (src, dst) in enumerate(
        (
            (w_any, w_s),
            (gate_any.at[0], gate_s),
            (up_any.at[0], up_s),
            (down_any.at[0], down_s.at[pl.ds(0, piece)]),
        )
    ):
        loads.append(pltpu.make_async_copy(src, dst, load_sem.at[i]))
        loads[-1].start()

    barrier = pltpu.get_barrier_semaphore()

    def greet_sp(i, carry):
        pl.semaphore_signal(
            barrier,
            inc=1,
            device_id=(lax.rem(sp + i, n_sp), tp),
            device_id_type=pl.DeviceIdType.MESH,
        )
        return carry

    def greet_tp(i, carry):
        pl.semaphore_signal(
            barrier,
            inc=1,
            device_id=(sp, lax.rem(tp + i, n_tp)),
            device_id_type=pl.DeviceIdType.MESH,
        )
        return carry

    lax.fori_loop(1, n_sp, greet_sp, 0)
    lax.fori_loop(1, n_tp, greet_tp, 0)

    before_gate = dot(decay_low[...], decay_matrix[...]) + decay_bias[...]
    logs = (
        jnp.minimum(before_gate, 0.0) - jnp.log1p(jnp.exp(-jnp.abs(before_gate)))
    ) / TEMPER + decay_shift[...]
    lower = iota((BLK, BLK), 0) >= iota((BLK, BLK), 1)
    lower_ones = jnp.where(lower, 1.0, 0.0).astype(BF)
    inside = []
    finals = []
    final_columns = []
    scaled_keys = []
    for n in range(2):
        block = slice(n * BLK, (n + 1) * BLK)
        high, middle, low = split3(logs[block])
        summed = dot(lower_ones, high) + (dot(lower_ones, middle) + dot(lower_ones, low))
        final = summed[BLK - 1 : BLK, :]
        keys = key_rows[block, :].astype(F32)
        end_keys = keys * jnp.exp(final - summed)
        high, low = split2(end_keys.T)
        update = dot(high, values[block, :]) + dot(low, values[block, :])
        update_s[n] = update
        inside.append(summed)
        finals.append(jnp.exp(final))
        final_columns.append(jnp.exp(jnp.broadcast_to(final, (BLK, hk)).T))
        scaled_keys.append(keys * jnp.exp(-summed))
    whole_decay = final_columns[0] * final_columns[1]
    for m in range(hv // BLK):
        lanes = slice(m * BLK, (m + 1) * BLK)
        state = update_s[0, :, lanes] * final_columns[1] + update_s[1, :, lanes]
        state_send[:, :, lanes] = state.reshape(n_sp, hk // n_sp, BLK).astype(BF)
    high, low = split2(whole_decay)
    packed = jnp.where(
        iota((hk, BLK), 1) < BLK // 2, high.astype(F32), low.astype(F32)
    )
    state_send[:, :, hv : hv + BLK] = packed.reshape(n_sp, hk // n_sp, BLK).astype(BF)

    pl.semaphore_wait(barrier, n_sp - 1 + n_tp - 1)

    def send_state(i, carry):
        peer = lax.rem(sp + i, n_sp)
        remote(
            state_send.at[peer], state_recv.at[sp], state_ss, state_rs.at[sp], (peer, tp)
        ).start()
        return carry

    lax.fori_loop(1, n_sp, send_state, 0)
    state_recv[sp] = state_send[sp]

    for n in range(2):
        block = slice(n * BLK, (n + 1) * BLK)
        query = queries[block, :].astype(F32) * jnp.exp(inside[n]) * hk**-0.5
        query_high, query_low = split2(query)
        key_high, key_low = split2(scaled_keys[n])
        scores = dot_nt(query_high, key_high) + (
            dot_nt(query_high, key_low) + dot_nt(query_low, key_high)
        )
        scores = jnp.where(lower, scores, 0.0)
        high, low = split2(scores)
        total = dot(high, values[block, :]) + dot(low, values[block, :])
        if n == 1:
            high, low = split2(update_s[0])
            total += dot(query_high, high) + (dot(query_high, low) + dot(query_low, high))
            query = query * finals[0]
        total_s[block, :] = total
        query_s[block, :] = query

    expert = iota((length, n_sp), 1)
    first = jnp.where(routes[:, 0:1] == expert, 1.0, 0.0)
    second = jnp.where(routes[:, 1:2] == expert, 1.0, 0.0)
    named = first + second
    earlier = jnp.where(iota((length, length), 0) > iota((length, length), 1), 1.0, 0.0)
    rank = dot(earlier.astype(BF), named.astype(BF))
    place = (named * (rank + 1.0)).astype(BF)
    count = n_sp * slots
    start = iota((count, n_sp), 1) * slots
    at = iota((count, n_sp), 0)
    spread = jnp.where((at >= start) & (at < start + slots), 1.0, 0.0).astype(BF)
    slot = ((iota((count, length), 0) & (slots - 1)) + 1).astype(F32)
    select_s[...] = jnp.where(dot_nt(spread, place) == slot, 1.0, 0.0).astype(BF)
    start = iota((n_sp, count), 0) * slots
    at = iota((n_sp, count), 1)
    spread = jnp.where((at >= start) & (at < start + slots), 1.0, 0.0).astype(BF)
    slot = ((iota((length, count), 1) & (slots - 1)) + 1).astype(F32)
    chosen = dot(place, spread) == slot
    high, low = split2(first * route_weights[:, 0:1] + second * route_weights[:, 1:2])
    weight_high[...] = jnp.where(chosen, dot(high, spread), 0.0).astype(BF)
    weight_low[...] = jnp.where(chosen, dot(low, spread), 0.0).astype(BF)

    for n in range(PARTS):
        row_recv[n, y] = jnp.zeros(row_recv.shape[2:], BF)
    down_s[piece:, :] = jnp.zeros((down_s.shape[0] - piece, width), BF)
    hidden_s[...] = jnp.zeros(hidden_s.shape, BF)

    def carry_state(j, state):
        prior_send[j] = state.astype(BF)

        @pl.when(j != sp)
        def _():
            remote(
                state_send.at[j], state_recv.at[j], state_ss, state_rs.at[j], (j, tp)
            ).wait_recv()
            remote(
                prior_send.at[j], prior_recv.at[sp], prior_ss, prior_rs, (j, tp)
            ).start()

        @pl.when(j == sp)
        def _():
            prior_recv[j] = state.astype(BF)

        came = state_recv[j].astype(F32)
        decay = came[:, hv : hv + 1] + came[:, hv + BLK // 2 : hv + BLK // 2 + 1]
        return state * decay + came[:, :hv]

    lax.fori_loop(0, n_sp, carry_state, jnp.zeros((hk // n_sp, hv), F32))
    most = pl.ds(0, n_sp - 1)
    remote(
        prior_send.at[most], prior_recv.at[most], prior_ss, prior_rs, mate
    ).wait_recv()
    carried = prior_recv[...].astype(F32).reshape(hk, hv).astype(BF)
    high, low = split2(query_s[...])
    total = total_s[...] + (dot(high, carried) + dot(low, carried))
    mixed = (
        total
        * lax.rsqrt(jnp.mean(total * total, axis=-1, keepdims=True) + EPSILON)
        * head_gain[...]
    ).astype(BF)
    mixed_s[...] = mixed.reshape(n_y, 2, rows, hv)

    def order(i):
        return jnp.where(
            lax.rem(i, 2) == 0, half_ring + lax.div(i, 2), half_ring - lax.div(i + 1, 2)
        )

    def pair_copy(n):
        return remote(
            pair_send.at[n], pair_recv.at[n], pair_ss.at[n], pair_rs.at[n], mate
        )

    def add_pair(n):
        pair_copy(n).wait_recv()
        total = own_s[n] + pair_recv[n].astype(F32)
        own_s[n] = total
        row_send[n] = total.astype(BF)

        def send_row(i, carry):
            yy = lax.rem(y + order(i), n_y)
            remote(
                row_send.at[n, yy],
                row_recv.at[n, y],
                row_ss.at[n],
                row_rs.at[n],
                (sp, 2 * yy + core),
            ).start()
            return carry

        lax.fori_loop(0, n_y - 1, send_row, 0)

    loads[0].wait()

    def project(n, carry):
        lanes = pl.ds(pl.multiple_of(n * part_width, part_width), part_width)
        theirs = mixed_s[:, other].reshape(n_y * rows, hv)
        pair_send[n] = dot(theirs, w_s[:, lanes]).astype(BF).reshape(n_y, rows, part_width)
        pair_copy(n).start()
        mine = mixed_s[:, core].reshape(n_y * rows, hv)
        product = dot(mine, w_s[:, lanes]).astype(BF).astype(F32)
        own_s[n] = product.reshape(n_y, rows, part_width)

        @pl.when(n > 0)
        def _():
            add_pair(n - 1)

        return carry

    lax.fori_loop(0, PARTS, project, 0)
    add_pair(PARTS - 1)

    rest = pl.ds(0, n_y - 1)
    for n in range(PARTS):
        lanes = slice(n * part_width, (n + 1) * part_width)
        remote(
            row_send.at[n, rest], row_recv.at[n, rest], row_ss.at[n], row_rs.at[n], mate
        ).wait_recv()
        total = own_s[n, y] + jnp.sum(row_recv[n].astype(F32), axis=0)
        mid_s[:, lanes] = stream[:, lanes].astype(F32) + total
    middle = mid_s[...]
    normed = (
        middle
        * lax.rsqrt(jnp.mean(middle * middle, axis=-1, keepdims=True) + EPSILON)
        * feed_gain[...]
    ).astype(BF)
    for j in range(n_tp):
        norm_send[j] = normed[:, j * columns : (j + 1) * columns]

    def to_tp(send, recv, send_sem, recv_sem):
        def start(i, carry):
            peer = lax.rem(tp + i, n_tp)
            remote(send.at[peer], recv.at[tp], send_sem, recv_sem, (sp, peer)).start()
            return carry

        lax.fori_loop(1, n_tp, start, 0)
        recv[tp] = send[tp]
        others = pl.ds(0, n_tp - 1)
        return remote(send.at[others], recv.at[others], send_sem, recv_sem, mate)

    norm_all = to_tp(norm_send, norm_recv, norm_ss, norm_rs)
    norm_all.wait_recv()
    group = norm_recv[...].reshape(length, columns)
    slot_send[...] = dot(select_s[...], group).astype(BF).reshape(n_sp, slots, columns)

    def send_slots(i, carry):
        peer = lax.rem(sp + i, n_sp)
        remote(
            slot_send.at[peer],
            rows_s.at[y, core, sp],
            slot_ss,
            slot_rs.at[sp],
            (peer, tp),
        ).start()
        return carry

    lax.fori_loop(1, n_sp, send_slots, 0)
    rows_s[y, core, sp] = slot_send[sp]

    n_half = n_sp // 2

    def ring_copy(d, step, p):
        yy = lax.rem(y + n_y + (1 - 2 * d) * (1 - step), n_y)
        to = lax.rem(y + n_y + 1 - 2 * d, n_y)
        part = rows_s.at[yy, core, pl.ds(p * n_half, n_half)]
        return remote(
            part, part, ring_ss.at[d, step, p], ring_rs.at[d, step, p], (sp, 2 * to + core)
        )

    def mate_copy(yy, c, p):
        part = rows_s.at[yy, c, pl.ds(p * n_half, n_half)]
        return remote(part, part, mate_ss.at[yy, p], mate_rs.at[yy, p], mate)

    for p in range(2):

        def wait_slots(b, carry):
            @pl.when(b != sp)
            def _():
                remote(
                    slot_send.at[b], rows_s.at[y, core, b], slot_ss, slot_rs.at[b], mate
                ).wait_recv()

            return carry

        lax.fori_loop(p * n_half, (p + 1) * n_half, wait_slots, 0)
        for d in range(2):
            if half_ring > 1 or d == p:
                ring_copy(d, 1, p).start()
        mate_copy(y, core, p).start()

    def pass_on(step):
        for p in range(2):
            for d in range(2):

                def one():
                    yy = lax.rem(y + n_y - (1 - 2 * d) * step, n_y)
                    ring_copy(d, step, p).wait_recv()
                    if d == p:
                        more = step < half_ring
                    else:
                        more = step + 1 < half_ring

                    @pl.when(more)
                    def _():
                        ring_copy(d, step + 1, p).start()

                    mate_copy(yy, core, p).start()

                if d == p:
                    one()
                else:
                    pl.when(step < half_ring)(one)

    loads[1].wait()
    loads[2].wait()
    loads[3].wait()
    gate_acc[...] = jnp.zeros(gate_acc.shape, F32)
    up_acc[...] = jnp.zeros(up_acc.shape, F32)

    def widen(m, carry):
        step = lax.div(m + 1, 2) + 1

        @pl.when(((m == 0) | (lax.rem(m, 2) == 1)) & (step <= half_ring))
        def _():
            pass_on(step)

        offset = jnp.where(lax.rem(m, 2) == 1, -lax.div(m + 1, 2), lax.div(m, 2))
        yy = lax.rem(y + n_y + offset, n_y)
        for p in range(2):
            mate_copy(yy, other, p).wait_recv()
        x = jnp.concatenate(
            [rows_s[yy, 0].reshape(count, columns), rows_s[yy, 1].reshape(count, columns)],
            axis=1,
        )
        depth = pl.ds(pl.multiple_of(yy * 2 * columns, 2 * columns), 2 * columns)
        gate_acc[...] += dot(x, gate_s[depth, :])
        up_acc[...] += dot(x, up_s[depth, :])
        return carry

    lax.fori_loop(0, n_y, widen, 0)
    gated = gate_acc[...]
    hidden = gated / (1.0 + jnp.exp(-gated)) * up_acc[...]
    hidden_s[:, 0:piece] = hidden.astype(BF)

    def half_copy(i):
        return remote(
            half_send.at[i], half_recv.at[i], half_ss.at[i], half_rs.at[i], mate
        )

    def add_half(i):
        yy = lax.rem(y + order(i), n_y)
        half_copy(i).wait_recv()
        total = half_own[i] + half_recv[i].astype(F32)
        half_own[i] = total

        @pl.when(i < n_y - 1)
        def _():
            sum_send[i] = total.astype(BF)
            remote(
                sum_send.at[i], sum_recv.at[y], sum_ss, sum_rs, (sp, 2 * yy + core)
            ).start()

    def lower_rows(i, carry):
        yy = lax.rem(y + order(i), n_y)
        lanes = pl.ds(pl.multiple_of(yy * 2 * columns, 2 * columns), 2 * columns)
        product = dot(hidden_s[...], down_s[:, lanes])
        left, right = product[:, :columns], product[:, columns:]
        half_send[i] = jnp.where(core == 0, right, left).astype(BF)
        half_copy(i).start()
        half_own[i] = jnp.where(core == 0, left, right).astype(BF).astype(F32)

        @pl.when(i > 0)
        def _():
            add_half(i - 1)

        return carry

    lax.fori_loop(0, n_y, lower_rows, 0)
    sum_recv[y] = jnp.zeros(sum_recv.shape[1:], BF)
    add_half(n_y - 1)
    remote(sum_send, sum_recv.at[rest], sum_ss, sum_rs, mate).wait_recv()
    total = half_own[n_y - 1] + jnp.sum(sum_recv[...].astype(F32), axis=0)
    back_send[...] = total.astype(BF).reshape(n_sp, slots, columns)

    def send_back(i, carry):
        peer = lax.rem(sp + i, n_sp)
        remote(back_send.at[peer], back_recv.at[sp], back_ss, back_rs, (peer, tp)).start()
        return carry

    lax.fori_loop(1, n_sp, send_back, 0)
    back_recv[sp] = back_send[sp]
    remote(back_send.at[most], back_recv.at[most], back_ss, back_rs, mate).wait_recv()
    returned = back_recv[...].reshape(count, columns)
    routed = dot(weight_high[...], returned) + dot(weight_low[...], returned)
    last_send[...] = routed.astype(BF).reshape(n_tp, rows, columns)
    last_all = to_tp(last_send, last_recv, last_ss, last_rs)
    last_all.wait_recv()
    for j in range(n_tp):
        lanes = slice(j * columns, (j + 1) * columns)
        out[:, lanes] = (mid_s[:, lanes] + last_recv[j].astype(F32)).astype(BF)

    remote(
        state_send.at[most], state_recv.at[most], state_ss, state_rs.at[0], mate
    ).wait_send()
    remote(prior_send.at[most], prior_recv.at[most], prior_ss, prior_rs, mate).wait_send()
    for n in range(PARTS):
        pair_copy(n).wait_send()
        remote(
            row_send.at[n, rest], row_recv.at[n, rest], row_ss.at[n], row_rs.at[n], mate
        ).wait_send()
    norm_all.wait_send()
    remote(
        slot_send.at[most], rows_s.at[0, 0, most], slot_ss, slot_rs.at[0], mate
    ).wait_send()
    for step in range(1, half_ring + 1):
        for d in range(2):
            for p in range(2):
                if step < half_ring or d == p:
                    ring_copy(d, step, p).wait_send()
    for yy in range(n_y):
        for p in range(2):
            mate_copy(yy, core, p).wait_send()
        half_copy(yy).wait_send()
    remote(sum_send, sum_recv.at[rest], sum_ss, sum_rs, mate).wait_send()
    remote(back_send.at[most], back_recv.at[most], back_ss, back_rs, mate).wait_send()
    last_all.wait_send()


def layer(
    n_sp,
    n_tp,
    stream_in,
    queries,
    key_rows,
    values,
    decay_low,
    decay_matrix,
    decay_bias,
    decay_shift,
    head_gain,
    output_matrix,
    feed_gain,
    routes,
    route_weights,
    expert_gate,
    specialist_widen,
    expert_down,
):
    rows, width = stream_in.shape
    length = queries.shape[0]
    hk, hv = queries.shape[1], values.shape[1]
    piece = expert_down.shape[1]
    n_y = n_tp // 2
    half_ring = n_y // 2
    slots = 2 * length // n_sp
    count = n_sp * slots
    columns = width // n_tp
    part = width // PARTS
    own = hk // n_sp
    padded = (piece + 127) // 128 * 128
    vmem, any_space = (
        pl.BlockSpec(memory_space=pltpu.VMEM),
        pl.BlockSpec(memory_space=pl.ANY),
    )
    dma = pltpu.SemaphoreType.DMA
    scratch = [
        pltpu.VMEM((hv, width), BF),
        pltpu.VMEM((width, piece), BF),
        pltpu.VMEM((width, piece), BF),
        pltpu.VMEM((padded, width), BF),
        pltpu.VMEM((length, hk), F32),
        pltpu.VMEM((length, hv), F32),
        pltpu.VMEM((2, hk, hv), F32),
        pltpu.VMEM((n_sp, own, hv + BLK), BF),
        pltpu.VMEM((n_sp, own, hv + BLK), BF),
        pltpu.VMEM((n_sp, own, hv), BF),
        pltpu.VMEM((n_sp, own, hv), BF),
        pltpu.VMEM((count, length), BF),
        pltpu.VMEM((length, count), BF),
        pltpu.VMEM((length, count), BF),
        pltpu.VMEM((n_y, 2, rows, hv), BF),
        pltpu.VMEM((PARTS, n_y, rows, part), BF),
        pltpu.VMEM((PARTS, n_y, rows, part), BF),
        pltpu.VMEM((PARTS, n_y, rows, part), F32),
        pltpu.VMEM((PARTS, n_y, rows, part), BF),
        pltpu.VMEM((PARTS, n_y, rows, part), BF),
        pltpu.VMEM((rows, width), F32),
        pltpu.VMEM((n_tp, rows, columns), BF),
        pltpu.VMEM((n_tp, rows, columns), BF),
        pltpu.VMEM((n_sp, slots, columns), BF),
        pltpu.VMEM((n_y, 2, n_sp, slots, columns), BF),
        pltpu.VMEM((count, piece), F32),
        pltpu.VMEM((count, piece), F32),
        pltpu.VMEM((count, padded), BF),
        pltpu.VMEM((n_y, count, columns), BF),
        pltpu.VMEM((n_y, count, columns), BF),
        pltpu.VMEM((n_y, count, columns), F32),
        pltpu.VMEM((n_y - 1, count, columns), BF),
        pltpu.VMEM((n_y, count, columns), BF),
        pltpu.VMEM((n_sp, slots, columns), BF),
        pltpu.VMEM((n_sp, slots, columns), BF),
        pltpu.VMEM((n_tp, rows, columns), BF),
        pltpu.VMEM((n_tp, rows, columns), BF),
        dma((4,)),
        dma,
        dma((n_sp,)),
        dma,
        dma,
        dma((PARTS,)),
        dma((PARTS,)),
        dma((PARTS,)),
        dma((PARTS,)),
        dma,
        dma,
        dma,
        dma((n_sp,)),
        dma((2, half_ring + 2, 2)),
        dma((2, half_ring + 2, 2)),
        dma((n_y, 2)),
        dma((n_y, 2)),
        dma((n_y,)),
        dma((n_y,)),
        dma,
        dma,
        dma,
        dma,
        dma,
        dma,
    ]
    return pl.pallas_call(
        functools.partial(layer_kernel, (n_sp, n_tp, rows, width, piece)),
        out_shape=jax.ShapeDtypeStruct((rows, width), BF),
        in_specs=[vmem] * 9 + [any_space] + [vmem] * 3 + [any_space] * 3,
        out_specs=vmem,
        scratch_shapes=scratch,
        compiler_params=pltpu.CompilerParams(
            collective_id=0, has_side_effects=True, vmem_limit_bytes=60 * 1024 * 1024
        ),
        name="layer",
    )(
        stream_in,
        queries,
        key_rows,
        values,
        decay_low,
        decay_matrix,
        decay_bias.reshape(1, -1),
        decay_shift,
        head_gain.reshape(1, -1),
        output_matrix,
        feed_gain.reshape(1, -1),
        routes,
        route_weights,
        expert_gate,
        specialist_widen,
        expert_down,
    )


def solution(mesh):
    in_specs = (
        P(("sp", "tp"), None),
        P("sp", "tp"),
        P("sp", "tp"),
        P("sp", "tp"),
        P("sp", None),
        P(None, "tp"),
        P("tp"),
        P("sp", "tp"),
        P(),
        P("tp", None),
        P(),
        P("sp", None),
        P("sp", None),
        P("sp", None, "tp"),
        P("sp", None, "tp"),
        P("sp", "tp", None),
    )
    return jax.shard_map(
        functools.partial(layer, mesh.shape["sp"], mesh.shape["tp"]),
        mesh=mesh,
        in_specs=in_specs,
        out_specs=P(("sp", "tp"), None),
        check_vma=False,
    )
```

```python
import functools

import jax
import jax.numpy as jnp
from jax import lax
from jax.experimental import pallas as pl
from jax.experimental.pallas import tpu as pltpu
from jax.sharding import PartitionSpec as P

BLK = 128
TEMPER = 16.0
EPSILON = 1e-06
PARTS = 4
BF = jnp.bfloat16
F32 = jnp.float32


def dot(a, b):
    return jnp.dot(a, b, preferred_element_type=F32)


def dot_nt(a, b):
    return lax.dot_general(a, b, (((1,), (1,)), ((), ())), preferred_element_type=F32)


def split2(x):
    high = x.astype(BF)
    return high, (x - high.astype(F32)).astype(BF)


def split3(x):
    high = x.astype(BF)
    rest = x - high.astype(F32)
    middle = rest.astype(BF)
    return high, middle, (rest - middle.astype(F32)).astype(BF)


def remote(src, dst, send_sem, recv_sem, device):
    return pltpu.make_async_remote_copy(
        src_ref=src,
        dst_ref=dst,
        send_sem=send_sem,
        recv_sem=recv_sem,
        device_id=device,
        device_id_type=pl.DeviceIdType.MESH,
    )


def iota(shape, dim):
    return lax.broadcasted_iota(jnp.int32, shape, dim)


def layer_kernel(
    size,
    stream,
    queries,
    key_rows,
    values,
    decay_low,
    decay_matrix,
    decay_bias,
    decay_shift,
    head_gain,
    w_any,
    feed_gain,
    routes,
    route_weights,
    gate_any,
    up_any,
    down_any,
    out,
    w_s,
    gate_s,
    up_s,
    down_s,
    query_s,
    total_s,
    update_s,
    state_send,
    state_recv,
    prior_send,
    prior_recv,
    select_s,
    weight_high,
    weight_low,
    mixed_s,
    pair_send,
    pair_recv,
    own_s,
    row_send,
    row_recv,
    mid_s,
    norm_send,
    norm_recv,
    slot_send,
    rows_s,
    gate_acc,
    up_acc,
    hidden_s,
    half_send,
    half_recv,
    half_own,
    sum_send,
    sum_recv,
    back_send,
    back_recv,
    last_send,
    last_recv,
    load_sem,
    state_ss,
    state_rs,
    prior_ss,
    prior_rs,
    pair_ss,
    pair_rs,
    row_ss,
    row_rs,
    norm_ss,
    norm_rs,
    slot_ss,
    slot_rs,
    ring_ss,
    ring_rs,
    mate_ss,
    mate_rs,
    half_ss,
    half_rs,
    sum_ss,
    sum_rs,
    back_ss,
    back_rs,
    last_ss,
    last_rs,
):
    n_sp, n_tp, rows, width, piece = size
    n_y = n_tp // 2
    half_ring = n_y // 2
    length = rows * n_tp
    slots = 2 * length // n_sp
    columns = width // n_tp
    part_width = width // PARTS
    hk = queries.shape[1]
    hv = values.shape[1]
    sp = lax.axis_index("sp")
    tp = lax.axis_index("tp")
    y = lax.div(tp, 2)
    core = lax.rem(tp, 2)
    other = 1 - core
    mate = (sp, tp + 1 - 2 * core)

    pending = []
    loads = []
    for i, (src, dst) in enumerate(
        (
            (w_any, w_s),
            (gate_any.at[0], gate_s),
            (up_any.at[0], up_s),
            (down_any.at[0], down_s.at[pl.ds(0, piece)]),
        )
    ):
        loads.append(pltpu.make_async_copy(src, dst, load_sem.at[i]))
        loads[-1].start()

    barrier = pltpu.get_barrier_semaphore()

    def greet_sp(i, carry):
        pl.semaphore_signal(
            barrier,
            inc=1,
            device_id=(lax.rem(sp + i, n_sp), tp),
            device_id_type=pl.DeviceIdType.MESH,
        )
        return carry

    def greet_tp(i, carry):
        pl.semaphore_signal(
            barrier,
            inc=1,
            device_id=(sp, lax.rem(tp + i, n_tp)),
            device_id_type=pl.DeviceIdType.MESH,
        )
        return carry

    lax.fori_loop(1, n_sp, greet_sp, 0)
    lax.fori_loop(1, n_tp, greet_tp, 0)

    line = iota((BLK, length), 0)
    lines = jnp.where(line == 0, decay_shift[...], 0.0)
    for i, row in enumerate((routes[0:1, :].astype(F32), routes[1:2, :].astype(F32))):
        lines = jnp.where(line == 1 + i, row, lines)
    for i in range(2):
        lines = jnp.where(line == 3 + i, route_weights[i : i + 1, :], lines)
    table = lines.T
    low_rows = decay_low[...].astype(F32).T.astype(BF)
    before_gate = dot(low_rows, decay_matrix[...]) + decay_bias[...]
    logs = (
        jnp.minimum(before_gate, 0.0) - jnp.log1p(jnp.exp(-jnp.abs(before_gate)))
    ) / TEMPER + table[:, 0:1]
    lower = iota((BLK, BLK), 0) >= iota((BLK, BLK), 1)
    lower_ones = jnp.where(lower, 1.0, 0.0).astype(BF)
    inside = []
    finals = []
    final_columns = []
    scaled_keys = []
    for n in range(2):
        block = slice(n * BLK, (n + 1) * BLK)
        high, middle, low = split3(logs[block])
        summed = dot(lower_ones, high) + (dot(lower_ones, middle) + dot(lower_ones, low))
        final = summed[BLK - 1 : BLK, :]
        keys = key_rows[block, :].astype(F32)
        end_keys = keys * jnp.exp(final - summed)
        high, low = split2(end_keys.T)
        update = dot(high, values[block, :]) + dot(low, values[block, :])
        update_s[n] = update
        inside.append(summed)
        finals.append(jnp.exp(final))
        final_columns.append(jnp.exp(jnp.broadcast_to(final, (BLK, hk)).T))
        scaled_keys.append(keys * jnp.exp(-summed))
    whole_decay = final_columns[0] * final_columns[1]
    for m in range(hv // BLK):
        lanes = slice(m * BLK, (m + 1) * BLK)
        state = update_s[0, :, lanes] * final_columns[1] + update_s[1, :, lanes]
        state_send[:, :, lanes] = state.reshape(n_sp, hk // n_sp, BLK).astype(BF)
    high, low = split2(whole_decay)
    packed = jnp.where(
        iota((hk, BLK), 1) < BLK // 2, high.astype(F32), low.astype(F32)
    )
    state_send[:, :, hv : hv + BLK] = packed.reshape(n_sp, hk // n_sp, BLK).astype(BF)

    pl.semaphore_wait(barrier, n_sp - 1 + n_tp - 1)

    def send_state(i, carry):
        peer = lax.rem(sp + i, n_sp)
        remote(
            state_send.at[peer], state_recv.at[sp], state_ss, state_rs.at[sp], (peer, tp)
        ).start()
        return carry

    lax.fori_loop(1, n_sp, send_state, 0)
    most = pl.ds(0, n_sp - 1)
    pending.append(
        remote(
            state_send.at[most], state_recv.at[most], state_ss, state_rs.at[0], mate
        ).wait_send
    )
    state_recv[sp] = state_send[sp]

    for n in range(2):
        block = slice(n * BLK, (n + 1) * BLK)
        query = queries[block, :].astype(F32) * jnp.exp(inside[n]) * hk**-0.5
        query_high, query_low = split2(query)
        key_high, key_low = split2(scaled_keys[n])
        scores = dot_nt(query_high, key_high) + (
            dot_nt(query_high, key_low) + dot_nt(query_low, key_high)
        )
        scores = jnp.where(lower, scores, 0.0)
        high, low = split2(scores)
        total = dot(high, values[block, :]) + dot(low, values[block, :])
        if n == 1:
            high, low = split2(update_s[0])
            total += dot(query_high, high) + (dot(query_high, low) + dot(query_low, high))
            query = query * finals[0]
        total_s[block, :] = total
        query_s[block, :] = query

    expert = iota((length, n_sp), 1).astype(F32)
    first = jnp.where(table[:, 1:2] == expert, 1.0, 0.0)
    second = jnp.where(table[:, 2:3] == expert, 1.0, 0.0)
    named = first + second
    earlier = jnp.where(iota((length, length), 0) > iota((length, length), 1), 1.0, 0.0)
    rank = dot(earlier.astype(BF), named.astype(BF))
    place = (named * (rank + 1.0)).astype(BF)
    count = n_sp * slots
    start = iota((count, n_sp), 1) * slots
    at = iota((count, n_sp), 0)
    spread = jnp.where((at >= start) & (at < start + slots), 1.0, 0.0).astype(BF)
    slot = ((iota((count, length), 0) & (slots - 1)) + 1).astype(F32)
    select_s[...] = jnp.where(dot_nt(spread, place) == slot, 1.0, 0.0).astype(BF)
    start = iota((n_sp, count), 0) * slots
    at = iota((n_sp, count), 1)
    spread = jnp.where((at >= start) & (at < start + slots), 1.0, 0.0).astype(BF)
    slot = ((iota((length, count), 1) & (slots - 1)) + 1).astype(F32)
    chosen = dot(place, spread) == slot
    high, low = split2(first * table[:, 3:4] + second * table[:, 4:5])
    weight_high[...] = jnp.where(chosen, dot(high, spread), 0.0).astype(BF)
    weight_low[...] = jnp.where(chosen, dot(low, spread), 0.0).astype(BF)

    down_s[piece:, :] = jnp.zeros((down_s.shape[0] - piece, width), BF)
    hidden_s[...] = jnp.zeros(hidden_s.shape, BF)

    def carry_state(j, state):
        prior_send[j] = state.astype(BF)

        @pl.when(j != sp)
        def _():
            remote(
                state_send.at[j], state_recv.at[j], state_ss, state_rs.at[j], (j, tp)
            ).wait_recv()
            remote(
                prior_send.at[j], prior_recv.at[sp], prior_ss, prior_rs, (j, tp)
            ).start()

        @pl.when(j == sp)
        def _():
            prior_recv[j] = state.astype(BF)

        came = state_recv[j].astype(F32)
        decay = came[:, hv : hv + 1] + came[:, hv + BLK // 2 : hv + BLK // 2 + 1]
        return state * decay + came[:, :hv]

    lax.fori_loop(0, n_sp, carry_state, jnp.zeros((hk // n_sp, hv), F32))
    prior_all = remote(
        prior_send.at[most], prior_recv.at[most], prior_ss, prior_rs, mate
    )
    prior_all.wait_recv()
    pending.append(prior_all.wait_send)
    carried = prior_recv[...].astype(F32).reshape(hk, hv).astype(BF)
    high, low = split2(query_s[...])
    total = total_s[...] + (dot(high, carried) + dot(low, carried))
    mixed = (
        total
        * lax.rsqrt(jnp.mean(total * total, axis=-1, keepdims=True) + EPSILON)
        * head_gain[...]
    ).astype(BF)
    mixed_s[...] = mixed.reshape(n_y, 2, rows, hv)

    def order(i):
        return jnp.where(
            lax.rem(i, 2) == 0, half_ring + lax.div(i, 2), half_ring - lax.div(i + 1, 2)
        )

    right = (sp, 2 * lax.rem(y + 1, n_y) + core)
    left = (sp, 2 * lax.rem(y + n_y - 1, n_y) + core)
    toward = (right, left)

    def pair_copy(n):
        return remote(
            pair_send.at[n], pair_recv.at[n], pair_ss.at[n], pair_rs.at[n], mate
        )

    def hop_copy(d, k, n):
        return remote(
            row_send.at[d, k, n],
            row_recv.at[d, k, n],
            row_ss.at[d, k, n],
            row_rs.at[d, k, n],
            toward[d],
        )

    def add_pair(n):
        pair_copy(n).wait_recv()
        own_s[n] = own_s[n] + pair_recv[n].astype(F32)
        far = own_s[n, lax.rem(y + half_ring, n_y)].astype(BF)
        for d in range(2):

            @pl.when(lax.div(n, PARTS // 2) == d)
            def _():
                row_send[d, 0, n] = far
                hop_copy(d, 0, n).start()

    loads[0].wait()

    def project(n, carry):
        lanes = pl.ds(pl.multiple_of(n * part_width, part_width), part_width)
        theirs = mixed_s[:, other].reshape(n_y * rows, hv)
        pair_send[n] = dot(theirs, w_s[:, lanes]).astype(BF).reshape(n_y, rows, part_width)
        pair_copy(n).start()
        mine = mixed_s[:, core].reshape(n_y * rows, hv)
        product = dot(mine, w_s[:, lanes]).astype(BF).astype(F32)
        own_s[n] = product.reshape(n_y, rows, part_width)

        @pl.when(n > 0)
        def _():
            add_pair(n - 1)

        return carry

    lax.fori_loop(0, PARTS, project, 0)
    add_pair(PARTS - 1)
    pending += [pair_copy(n).wait_send for n in range(PARTS)]

    def pass_rows(k, carry):
        for n in range(PARTS):
            for d in range(2):
                hold = lax.rem(y + n_y + (1 - 2 * d) * (half_ring - k), n_y)
                comes = n // (PARTS // 2) == d

                @pl.when(jnp.logical_or(k > 1, comes))
                def _():
                    hop_copy(d, k - 1, n).wait_recv()
                    total = own_s[n, hold] + row_recv[d, k - 1, n].astype(F32)
                    row_send[d, k, n] = total.astype(BF)

                if not comes:

                    @pl.when(k == 1)
                    def _():
                        row_send[d, k, n] = own_s[n, hold].astype(BF)

                hop_copy(d, k, n).start()
        return carry

    lax.fori_loop(1, half_ring, pass_rows, 0)
    for n in range(PARTS):
        lanes = slice(n * part_width, (n + 1) * part_width)
        total = own_s[n, y]
        for d in range(2):
            if half_ring > 1 or n // (PARTS // 2) == d:
                hop_copy(d, half_ring - 1, n).wait_recv()
                total += row_recv[d, half_ring - 1, n].astype(F32)
            for k in range(half_ring):
                if k > 0 or n // (PARTS // 2) == d:
                    pending.append(hop_copy(d, k, n).wait_send)
        mid_s[:, lanes] = stream[:, lanes].astype(F32) + total
    middle = mid_s[...]
    normed = (
        middle
        * lax.rsqrt(jnp.mean(middle * middle, axis=-1, keepdims=True) + EPSILON)
        * feed_gain[...]
    ).astype(BF)
    for j in range(n_tp):
        norm_send[j] = normed[:, j * columns : (j + 1) * columns]

    def to_tp(send, recv, send_sem, recv_sem):
        def start(i, carry):
            peer = lax.rem(tp + i, n_tp)
            remote(send.at[peer], recv.at[tp], send_sem, recv_sem, (sp, peer)).start()
            return carry

        lax.fori_loop(1, n_tp, start, 0)
        recv[tp] = send[tp]
        others = pl.ds(0, n_tp - 1)
        return remote(send.at[others], recv.at[others], send_sem, recv_sem, mate)

    norm_all = to_tp(norm_send, norm_recv, norm_ss, norm_rs)
    pending.append(norm_all.wait_send)
    norm_all.wait_recv()
    group = norm_recv[...].reshape(length, columns)
    slot_send[...] = dot(select_s[...], group).astype(BF).reshape(n_sp, slots, columns)

    def send_slots(i, carry):
        peer = lax.rem(sp + i, n_sp)
        remote(
            slot_send.at[peer],
            rows_s.at[y, core, sp],
            slot_ss,
            slot_rs.at[sp],
            (peer, tp),
        ).start()
        return carry

    lax.fori_loop(1, n_sp, send_slots, 0)
    pending.append(
        remote(
            slot_send.at[most], rows_s.at[0, 0, most], slot_ss, slot_rs.at[0], mate
        ).wait_send
    )
    rows_s[y, core, sp] = slot_send[sp]

    n_half = n_sp // 2

    def ring_copy(d, step, p):
        yy = lax.rem(y + n_y + (1 - 2 * d) * (1 - step), n_y)
        to = lax.rem(y + n_y + 1 - 2 * d, n_y)
        part = rows_s.at[yy, core, pl.ds(p * n_half, n_half)]
        return remote(
            part, part, ring_ss.at[d, step, p], ring_rs.at[d, step, p], (sp, 2 * to + core)
        )

    def mate_copy(yy, c, p):
        part = rows_s.at[yy, c, pl.ds(p * n_half, n_half)]
        return remote(part, part, mate_ss.at[yy, p], mate_rs.at[yy, p], mate)

    for p in range(2):

        def wait_slots(b, carry):
            @pl.when(b != sp)
            def _():
                remote(
                    slot_send.at[b], rows_s.at[y, core, b], slot_ss, slot_rs.at[b], mate
                ).wait_recv()

            return carry

        lax.fori_loop(p * n_half, (p + 1) * n_half, wait_slots, 0)
        for d in range(2):
            if half_ring > 1 or d == p:
                ring_copy(d, 1, p).start()
        mate_copy(y, core, p).start()

    def pass_on(step):
        for p in range(2):
            for d in range(2):

                def one():
                    yy = lax.rem(y + n_y - (1 - 2 * d) * step, n_y)
                    ring_copy(d, step, p).wait_recv()
                    if d == p:
                        more = step < half_ring
                    else:
                        more = step + 1 < half_ring

                    @pl.when(more)
                    def _():
                        ring_copy(d, step + 1, p).start()

                    mate_copy(yy, core, p).start()

                if d == p:
                    one()
                else:
                    pl.when(step < half_ring)(one)

    for step in range(1, half_ring + 1):
        for d in range(2):
            for p in range(2):
                if step < half_ring or d == p:
                    pending.append(ring_copy(d, step, p).wait_send)
    for i in range(n_y):
        for p in range(2):
            pending.append(mate_copy(i, core, p).wait_send)
    for load in loads[1:]:
        load.wait()
    gate_acc[...] = jnp.zeros(gate_acc.shape, F32)
    up_acc[...] = jnp.zeros(up_acc.shape, F32)

    def widen(m, carry):
        step = lax.div(m + 1, 2) + 1

        @pl.when(((m == 0) | (lax.rem(m, 2) == 1)) & (step <= half_ring))
        def _():
            pass_on(step)

        offset = jnp.where(lax.rem(m, 2) == 1, -lax.div(m + 1, 2), lax.div(m, 2))
        yy = lax.rem(y + n_y + offset, n_y)
        for p in range(2):
            mate_copy(yy, other, p).wait_recv()
        x = jnp.concatenate(
            [rows_s[yy, 0].reshape(count, columns), rows_s[yy, 1].reshape(count, columns)],
            axis=1,
        )
        depth = pl.ds(pl.multiple_of(yy * 2 * columns, 2 * columns), 2 * columns)
        gate_acc[...] += dot_nt(x, gate_s[:, depth])
        up_acc[...] += dot_nt(x, up_s[:, depth])
        return carry

    lax.fori_loop(0, n_y, widen, 0)
    gated = gate_acc[...]
    hidden = gated / (1.0 + jnp.exp(-gated)) * up_acc[...]
    hidden_s[:, 0:piece] = hidden.astype(BF)

    def half_copy(i):
        return remote(
            half_send.at[i], half_recv.at[i], half_ss.at[i], half_rs.at[i], mate
        )

    def sum_copy(d, k, p):
        to = lax.rem(y + n_y + 1 - 2 * d, n_y)
        return remote(
            sum_send.at[d, k, p],
            sum_recv.at[d, k, p],
            sum_ss.at[d, k, p],
            sum_rs.at[d, k, p],
            (sp, 2 * to + core),
        )

    def add_half(i):
        half_copy(i).wait_recv()

        @pl.when(i == 0)
        def _():
            for p in range(2):
                total = half_own[i, p] + half_recv[i, p].astype(F32)
                sum_send[p, 0, p] = total.astype(BF)
                sum_copy(p, 0, p).start()

        @pl.when(i > 0)
        def _():
            d = 1 - lax.rem(i, 2)
            k = lax.div(i + 1, 2)
            for p in range(2):
                total = half_own[i, p] + half_recv[i, p].astype(F32)

                @pl.when(jnp.logical_or(k > 1, d == p))
                def _():
                    sum_copy(d, k - 1, p).wait_recv()
                    more = total + sum_recv[d, k - 1, p].astype(F32)
                    sum_send[d, k, p] = more.astype(BF)

                @pl.when(jnp.logical_and(k == 1, d != p))
                def _():
                    sum_send[d, k, p] = total.astype(BF)

                sum_copy(d, k, p).start()

    def lower_rows(i, carry):
        yy = lax.rem(y + order(i), n_y)
        lanes = pl.ds(pl.multiple_of(yy * 2 * columns, 2 * columns), 2 * columns)
        product = dot(hidden_s[...], down_s[:, lanes])
        left, right = product[:, :columns], product[:, columns:]
        shape = half_send.shape[1:]
        half_send[i] = jnp.where(core == 0, right, left).astype(BF).reshape(shape)
        half_copy(i).start()
        half_own[i] = jnp.where(core == 0, left, right).reshape(shape)

        @pl.when(i > 0)
        def _():
            add_half(i - 1)

        return carry

    lax.fori_loop(0, n_y, lower_rows, 0)
    last = n_y - 1
    half_copy(last).wait_recv()
    for p in range(2):
        total = half_own[last, p] + half_recv[last, p].astype(F32)
        for d in range(2):
            if half_ring > 1 or d == p:
                sum_copy(d, half_ring - 1, p).wait_recv()
                total += sum_recv[d, half_ring - 1, p].astype(F32)
        back_send[p * n_half : (p + 1) * n_half] = total.astype(BF).reshape(
            n_half, slots, columns
        )
    for i in range(n_y):
        pending.append(half_copy(i).wait_send)
    for d in range(2):
        for k in range(half_ring):
            for p in range(2):
                if k > 0 or d == p:
                    pending.append(sum_copy(d, k, p).wait_send)

    def send_back(i, carry):
        peer = lax.rem(sp + i, n_sp)
        remote(back_send.at[peer], back_recv.at[sp], back_ss, back_rs, (peer, tp)).start()
        return carry

    lax.fori_loop(1, n_sp, send_back, 0)
    back_recv[sp] = back_send[sp]
    back_all = remote(back_send.at[most], back_recv.at[most], back_ss, back_rs, mate)
    pending.append(back_all.wait_send)
    back_all.wait_recv()
    returned = back_recv[...].reshape(count, columns)
    routed = dot(weight_high[...], returned) + dot(weight_low[...], returned)
    last_send[...] = routed.astype(BF).reshape(n_tp, rows, columns)
    last_all = to_tp(last_send, last_recv, last_ss, last_rs)
    pending.append(last_all.wait_send)
    last_all.wait_recv()
    for j in range(n_tp):
        lanes = slice(j * columns, (j + 1) * columns)
        out[:, lanes] = (mid_s[:, lanes] + last_recv[j].astype(F32)).astype(BF)

    for finish in pending:
        finish()


def layer(
    n_sp,
    n_tp,
    stream_in,
    queries,
    key_rows,
    values,
    decay_low,
    decay_matrix,
    decay_bias,
    decay_shift,
    head_gain,
    output_matrix,
    feed_gain,
    routes,
    route_weights,
    expert_gate,
    specialist_widen,
    expert_down,
):
    rows, width = stream_in.shape
    length = queries.shape[0]
    hk, hv = queries.shape[1], values.shape[1]
    piece = expert_down.shape[1]
    n_y = n_tp // 2
    half_ring = n_y // 2
    slots = 2 * length // n_sp
    count = n_sp * slots
    columns = width // n_tp
    part = width // PARTS
    own = hk // n_sp
    padded = (piece + 127) // 128 * 128
    vmem, any_space = (
        pl.BlockSpec(memory_space=pltpu.VMEM),
        pl.BlockSpec(memory_space=pl.ANY),
    )
    dma = pltpu.SemaphoreType.DMA
    scratch = [
        pltpu.VMEM((hv, width), BF),
        pltpu.VMEM((piece, width), BF),
        pltpu.VMEM((piece, width), BF),
        pltpu.VMEM((padded, width), BF),
        pltpu.VMEM((length, hk), F32),
        pltpu.VMEM((length, hv), F32),
        pltpu.VMEM((2, hk, hv), F32),
        pltpu.VMEM((n_sp, own, hv + BLK), BF),
        pltpu.VMEM((n_sp, own, hv + BLK), BF),
        pltpu.VMEM((n_sp, own, hv), BF),
        pltpu.VMEM((n_sp, own, hv), BF),
        pltpu.VMEM((count, length), BF),
        pltpu.VMEM((length, count), BF),
        pltpu.VMEM((length, count), BF),
        pltpu.VMEM((n_y, 2, rows, hv), BF),
        pltpu.VMEM((PARTS, n_y, rows, part), BF),
        pltpu.VMEM((PARTS, n_y, rows, part), BF),
        pltpu.VMEM((PARTS, n_y, rows, part), F32),
        pltpu.VMEM((2, half_ring, PARTS, rows, part), BF),
        pltpu.VMEM((2, half_ring, PARTS, rows, part), BF),
        pltpu.VMEM((rows, width), F32),
        pltpu.VMEM((n_tp, rows, columns), BF),
        pltpu.VMEM((n_tp, rows, columns), BF),
        pltpu.VMEM((n_sp, slots, columns), BF),
        pltpu.VMEM((n_y, 2, n_sp, slots, columns), BF),
        pltpu.VMEM((count, piece), F32),
        pltpu.VMEM((count, piece), F32),
        pltpu.VMEM((count, padded), BF),
        pltpu.VMEM((n_y, 2, count // 2, columns), BF),
        pltpu.VMEM((n_y, 2, count // 2, columns), BF),
        pltpu.VMEM((n_y, 2, count // 2, columns), F32),
        pltpu.VMEM((2, half_ring, 2, count // 2, columns), BF),
        pltpu.VMEM((2, half_ring, 2, count // 2, columns), BF),
        pltpu.VMEM((n_sp, slots, columns), BF),
        pltpu.VMEM((n_sp, slots, columns), BF),
        pltpu.VMEM((n_tp, rows, columns), BF),
        pltpu.VMEM((n_tp, rows, columns), BF),
        dma((4,)),
        dma,
        dma((n_sp,)),
        dma,
        dma,
        dma((PARTS,)),
        dma((PARTS,)),
        dma((2, half_ring, PARTS)),
        dma((2, half_ring, PARTS)),
        dma,
        dma,
        dma,
        dma((n_sp,)),
        dma((2, half_ring + 2, 2)),
        dma((2, half_ring + 2, 2)),
        dma((n_y, 2)),
        dma((n_y, 2)),
        dma((n_y,)),
        dma((n_y,)),
        dma((2, half_ring, 2)),
        dma((2, half_ring, 2)),
        dma,
        dma,
        dma,
        dma,
    ]
    return pl.pallas_call(
        functools.partial(layer_kernel, (n_sp, n_tp, rows, width, piece)),
        out_shape=jax.ShapeDtypeStruct((rows, width), BF),
        in_specs=[vmem] * 9 + [any_space] + [vmem] * 3 + [any_space] * 3,
        out_specs=vmem,
        scratch_shapes=scratch,
        compiler_params=pltpu.CompilerParams(
            collective_id=0, has_side_effects=True, vmem_limit_bytes=60 * 1024 * 1024
        ),
        name="layer",
    )(
        stream_in,
        queries,
        key_rows,
        values,
        decay_low.T,
        decay_matrix,
        decay_bias.reshape(1, -1),
        decay_shift.T,
        head_gain.reshape(1, -1),
        output_matrix,
        feed_gain.reshape(1, -1),
        routes.T,
        route_weights.T,
        jnp.swapaxes(expert_gate, 1, 2),
        jnp.swapaxes(specialist_widen, 1, 2),
        expert_down,
    )


def solution(mesh):
    in_specs = (
        P(("sp", "tp"), None),
        P("sp", "tp"),
        P("sp", "tp"),
        P("sp", "tp"),
        P("sp", None),
        P(None, "tp"),
        P("tp"),
        P("sp", "tp"),
        P(),
        P("tp", None),
        P(),
        P("sp", None),
        P("sp", None),
        P("sp", None, "tp"),
        P("sp", None, "tp"),
        P("sp", "tp", None),
    )
    return jax.shard_map(
        functools.partial(layer, mesh.shape["sp"], mesh.shape["tp"]),
        mesh=mesh,
        in_specs=in_specs,
        out_specs=P(("sp", "tp"), None),
        check_vma=False,
    )
```

```python
import functools

import jax
import jax.numpy as jnp
from jax import lax
from jax.experimental import pallas as pl
from jax.experimental.pallas import tpu as pltpu
from jax.sharding import PartitionSpec as P

BLK = 128
TEMPER = 16.0
EPSILON = 1e-06
PIECES = 4
BF = jnp.bfloat16
F32 = jnp.float32


def dot(a, b):
    return jnp.dot(a, b, preferred_element_type=F32)


def dot_nt(a, b):
    return lax.dot_general(a, b, (((1,), (1,)), ((), ())), preferred_element_type=F32)


def split2(x):
    high = x.astype(BF)
    return high, (x - high.astype(F32)).astype(BF)


def split3(x):
    high = x.astype(BF)
    rest = x - high.astype(F32)
    middle = rest.astype(BF)
    return high, middle, (rest - middle.astype(F32)).astype(BF)


def remote(src, dst, send_sem, recv_sem, device):
    return pltpu.make_async_remote_copy(
        src_ref=src,
        dst_ref=dst,
        send_sem=send_sem,
        recv_sem=recv_sem,
        device_id=device,
        device_id_type=pl.DeviceIdType.MESH,
    )


def iota(shape, dim):
    return lax.broadcasted_iota(jnp.int32, shape, dim)


def layer_kernel(
    size,
    stream,
    queries,
    key_rows,
    values,
    decay_low,
    decay_matrix,
    decay_bias,
    decay_shift,
    head_gain,
    w_any,
    feed_gain,
    routes,
    route_weights,
    gate_any,
    up_any,
    down_any,
    out,
    w_s,
    gate_s,
    up_s,
    down_s,
    query_s,
    total_s,
    update_s,
    state_send,
    state_recv,
    prior_send,
    prior_recv,
    select_s,
    weight_high,
    weight_low,
    mixed_s,
    first_send,
    first_recv,
    row_send,
    row_recv,
    row_own,
    row_out,
    row_in,
    mid_s,
    square_send,
    square_recv,
    scale_send,
    scale_recv,
    slot_send,
    rows_s,
    gate_acc,
    up_acc,
    hidden_s,
    half_send,
    half_recv,
    half_own,
    sum_out,
    sum_in,
    back_send,
    back_recv,
    last_send,
    last_recv,
    load_sem,
    state_ss,
    state_rs,
    prior_ss,
    prior_rs,
    first_ss,
    first_rs,
    row_ss,
    row_rs,
    hop_ss,
    hop_rs,
    square_ss,
    square_rs,
    scale_ss,
    scale_rs,
    slot_ss,
    slot_rs,
    ring_ss,
    ring_rs,
    mate_ss,
    mate_rs,
    half_ss,
    half_rs,
    sum_ss,
    sum_rs,
    back_ss,
    back_rs,
    last_ss,
    last_rs,
):
    n_sp, n_tp, rows, width, piece = size
    n_y = n_tp // 2
    half_ring = n_y // 2
    length = rows * n_tp
    slots = 2 * length // n_sp
    columns = width // n_tp
    count = n_sp * slots
    pieces = min(PIECES, n_sp)
    hk = queries.shape[1]
    hv = values.shape[1]
    sp = lax.axis_index("sp")
    tp = lax.axis_index("tp")
    y = lax.div(tp, 2)
    core = lax.rem(tp, 2)
    other = 1 - core
    mate = (sp, tp + 1 - 2 * core)

    pending = []
    loads = []
    for i, (src, dst) in enumerate(
        (
            (w_any, w_s),
            (gate_any.at[0], gate_s),
            (up_any.at[0], up_s),
            (down_any.at[0], down_s.at[pl.ds(0, piece)]),
        )
    ):
        loads.append(pltpu.make_async_copy(src, dst, load_sem.at[i]))
        loads[-1].start()

    barrier = pltpu.get_barrier_semaphore()

    def greet_sp(i, carry):
        pl.semaphore_signal(
            barrier,
            inc=1,
            device_id=(lax.rem(sp + i, n_sp), tp),
            device_id_type=pl.DeviceIdType.MESH,
        )
        return carry

    def greet_tp(i, carry):
        pl.semaphore_signal(
            barrier,
            inc=1,
            device_id=(sp, lax.rem(tp + i, n_tp)),
            device_id_type=pl.DeviceIdType.MESH,
        )
        return carry

    lax.fori_loop(1, n_sp, greet_sp, 0)
    lax.fori_loop(1, n_tp, greet_tp, 0)

    line = iota((BLK, length), 0)
    lines = jnp.where(line == 0, decay_shift[...], 0.0)
    for i, row in enumerate((routes[0:1, :].astype(F32), routes[1:2, :].astype(F32))):
        lines = jnp.where(line == 1 + i, row, lines)
    for i in range(2):
        lines = jnp.where(line == 3 + i, route_weights[i : i + 1, :], lines)
    table = lines.T
    low_rows = decay_low[...].astype(F32).T.astype(BF)
    before_gate = dot(low_rows, decay_matrix[...]) + decay_bias[...]
    logs = (
        jnp.minimum(before_gate, 0.0) - jnp.log1p(jnp.exp(-jnp.abs(before_gate)))
    ) / TEMPER + table[:, 0:1]
    lower = iota((BLK, BLK), 0) >= iota((BLK, BLK), 1)
    lower_ones = jnp.where(lower, 1.0, 0.0).astype(BF)
    inside = []
    finals = []
    final_columns = []
    scaled_keys = []
    for n in range(2):
        block = slice(n * BLK, (n + 1) * BLK)
        high, middle, low = split3(logs[block])
        summed = dot(lower_ones, high) + (dot(lower_ones, middle) + dot(lower_ones, low))
        final = summed[BLK - 1 : BLK, :]
        keys = key_rows[block, :].astype(F32)
        end_keys = keys * jnp.exp(final - summed)
        high, low = split2(end_keys.T)
        update = dot(high, values[block, :]) + dot(low, values[block, :])
        update_s[n] = update
        inside.append(summed)
        finals.append(jnp.exp(final))
        final_columns.append(jnp.exp(jnp.broadcast_to(final, (BLK, hk)).T))
        scaled_keys.append(keys * jnp.exp(-summed))
    whole_decay = final_columns[0] * final_columns[1]
    for m in range(hv // BLK):
        lanes = slice(m * BLK, (m + 1) * BLK)
        state = update_s[0, :, lanes] * final_columns[1] + update_s[1, :, lanes]
        state_send[:, :, lanes] = state.reshape(n_sp, hk // n_sp, BLK).astype(BF)
    high, low = split2(whole_decay)
    packed = jnp.where(
        iota((hk, BLK), 1) < BLK // 2, high.astype(F32), low.astype(F32)
    )
    state_send[:, :, hv : hv + BLK] = packed.reshape(n_sp, hk // n_sp, BLK).astype(BF)

    for j in range(n_tp):
        first_send[j] = stream[:, j * columns : (j + 1) * columns]
    pl.semaphore_wait(barrier, n_sp - 1 + n_tp - 1)

    def send_state(i, carry):
        peer = lax.rem(sp + i, n_sp)
        remote(
            state_send.at[peer], state_recv.at[sp], state_ss, state_rs.at[sp], (peer, tp)
        ).start()
        return carry

    lax.fori_loop(1, n_sp, send_state, 0)
    most = pl.ds(0, n_sp - 1)
    pending.append(
        remote(
            state_send.at[most], state_recv.at[most], state_ss, state_rs.at[0], mate
        ).wait_send
    )
    state_recv[sp] = state_send[sp]

    def to_tp(send, recv, send_sem, recv_sem):
        def start(i, carry):
            peer = lax.rem(tp + i, n_tp)
            remote(send.at[peer], recv.at[tp], send_sem, recv_sem, (sp, peer)).start()
            return carry

        lax.fori_loop(1, n_tp, start, 0)
        recv[tp] = send[tp]
        others = pl.ds(0, n_tp - 1)
        every = remote(send.at[others], recv.at[others], send_sem, recv_sem, mate)
        pending.append(every.wait_send)
        return every

    def to_sp(send, recv, send_sem, recv_sem):
        def start(i, carry):
            peer = lax.rem(sp + i, n_sp)
            remote(send.at[peer], recv.at[sp], send_sem, recv_sem, (peer, tp)).start()
            return carry

        lax.fori_loop(1, n_sp, start, 0)
        recv[sp] = send[sp]
        every = remote(send.at[most], recv.at[most], send_sem, recv_sem, mate)
        pending.append(every.wait_send)
        return every

    first_all = to_tp(first_send, first_recv, first_ss, first_rs)

    for n in range(2):
        block = slice(n * BLK, (n + 1) * BLK)
        query = queries[block, :].astype(F32) * jnp.exp(inside[n]) * hk**-0.5
        query_high, query_low = split2(query)
        key_high, key_low = split2(scaled_keys[n])
        scores = dot_nt(query_high, key_high) + (
            dot_nt(query_high, key_low) + dot_nt(query_low, key_high)
        )
        scores = jnp.where(lower, scores, 0.0)
        high, low = split2(scores)
        total = dot(high, values[block, :]) + dot(low, values[block, :])
        if n == 1:
            high, low = split2(update_s[0])
            total += dot(query_high, high) + (dot(query_high, low) + dot(query_low, high))
            query = query * finals[0]
        total_s[block, :] = total
        query_s[block, :] = query

    expert = iota((length, n_sp), 1).astype(F32)
    first = jnp.where(table[:, 1:2] == expert, 1.0, 0.0)
    second = jnp.where(table[:, 2:3] == expert, 1.0, 0.0)
    named = first + second
    earlier = jnp.where(iota((length, length), 0) > iota((length, length), 1), 1.0, 0.0)
    rank = dot(earlier.astype(BF), named.astype(BF))
    place = (named * (rank + 1.0)).astype(BF)
    start = iota((count, n_sp), 1) * slots
    at = iota((count, n_sp), 0)
    spread = jnp.where((at >= start) & (at < start + slots), 1.0, 0.0).astype(BF)
    slot = ((iota((count, length), 0) & (slots - 1)) + 1).astype(F32)
    select_s[...] = jnp.where(dot_nt(spread, place) == slot, 1.0, 0.0).astype(BF)
    start = iota((n_sp, count), 0) * slots
    at = iota((n_sp, count), 1)
    spread = jnp.where((at >= start) & (at < start + slots), 1.0, 0.0).astype(BF)
    slot = ((iota((length, count), 1) & (slots - 1)) + 1).astype(F32)
    chosen = dot(place, spread) == slot
    high, low = split2(first * table[:, 3:4] + second * table[:, 4:5])
    weight_high[...] = jnp.where(chosen, dot(high, spread), 0.0).astype(BF)
    weight_low[...] = jnp.where(chosen, dot(low, spread), 0.0).astype(BF)

    down_s[piece:, :] = jnp.zeros((down_s.shape[0] - piece, width), BF)
    hidden_s[...] = jnp.zeros(hidden_s.shape, BF)

    def carry_state(j, state):
        prior_send[j] = state.astype(BF)

        @pl.when(j != sp)
        def _():
            remote(
                state_send.at[j], state_recv.at[j], state_ss, state_rs.at[j], (j, tp)
            ).wait_recv()
            remote(
                prior_send.at[j], prior_recv.at[sp], prior_ss, prior_rs, (j, tp)
            ).start()

        @pl.when(j == sp)
        def _():
            prior_recv[j] = state.astype(BF)

        came = state_recv[j].astype(F32)
        decay = came[:, hv : hv + 1] + came[:, hv + BLK // 2 : hv + BLK // 2 + 1]
        return state * decay + came[:, :hv]

    lax.fori_loop(0, n_sp, carry_state, jnp.zeros((hk // n_sp, hv), F32))
    prior_all = remote(
        prior_send.at[most], prior_recv.at[most], prior_ss, prior_rs, mate
    )
    prior_all.wait_recv()
    pending.append(prior_all.wait_send)
    carried = prior_recv[...].astype(F32).reshape(hk, hv).astype(BF)
    high, low = split2(query_s[...])
    total = total_s[...] + (dot(high, carried) + dot(low, carried))
    mixed = (
        total
        * lax.rsqrt(jnp.mean(total * total, axis=-1, keepdims=True) + EPSILON)
        * head_gain[...]
    ).astype(BF)
    mixed_s[...] = mixed

    def order(i):
        return jnp.where(
            lax.rem(i, 2) == 0, half_ring + lax.div(i, 2), half_ring - lax.div(i + 1, 2)
        )

    def summed_product(left_ref, right_ref, send, recv, own, out_buf, in_buf, sems):
        mate_send, mate_recv, hop_send, hop_recv = sems
        shape = send.shape[1:]
        first_way = shape[0] // 2

        def share(i):
            return remote(send.at[i], recv.at[i], mate_send.at[i], mate_recv.at[i], mate)

        def hop(d, k, p):
            to = lax.rem(y + n_y + 1 - 2 * d, n_y)
            return remote(
                out_buf.at[d, k, p],
                in_buf.at[d, k, p],
                hop_send.at[d, k, p],
                hop_recv.at[d, k, p],
                (sp, 2 * to + core),
            )

        def add(i):
            share(i).wait_recv()

            @pl.when(i == 0)
            def _():
                for p in range(shape[0]):
                    d = p // first_way
                    total = own[i, p] + recv[i, p].astype(F32)
                    out_buf[d, 0, p] = total.astype(BF)
                    hop(d, 0, p).start()

            @pl.when(i > 0)
            def _():
                d = 1 - lax.rem(i, 2)
                k = lax.div(i + 1, 2)
                for p in range(shape[0]):
                    total = own[i, p] + recv[i, p].astype(F32)
                    comes = jnp.logical_or(k > 1, d == p // first_way)

                    @pl.when(comes)
                    def _():
                        hop(d, k - 1, p).wait_recv()
                        more = total + in_buf[d, k - 1, p].astype(F32)
                        out_buf[d, k, p] = more.astype(BF)

                    @pl.when(jnp.logical_not(comes))
                    def _():
                        out_buf[d, k, p] = total.astype(BF)

                    hop(d, k, p).start()

        def multiply(i, carry):
            yy = lax.rem(y + order(i), n_y)
            lanes = pl.ds(pl.multiple_of(yy * 2 * columns, 2 * columns), 2 * columns)
            product = dot(left_ref[...], right_ref[:, lanes])
            low, high = product[:, :columns], product[:, columns:]
            send[i] = jnp.where(core == 0, high, low).astype(BF).reshape(shape)
            share(i).start()
            own[i] = jnp.where(core == 0, low, high).reshape(shape)

            @pl.when(i > 0)
            def _():
                add(i - 1)

            return carry

        lax.fori_loop(0, n_y, multiply, 0)
        last = n_y - 1
        share(last).wait_recv()
        totals = []
        for p in range(shape[0]):
            total = own[last, p] + recv[last, p].astype(F32)
            for d in range(2):
                if half_ring > 1 or d == p // first_way:
                    hop(d, half_ring - 1, p).wait_recv()
                    total += in_buf[d, half_ring - 1, p].astype(F32)
            totals.append(total)
        for i in range(n_y):
            pending.append(share(i).wait_send)
        for d in range(2):
            for k in range(half_ring):
                for p in range(shape[0]):
                    if k > 0 or d == p // first_way:
                        pending.append(hop(d, k, p).wait_send)
        return jnp.concatenate(totals, axis=0)

    loads[0].wait()
    attended = summed_product(
        mixed_s,
        w_s,
        row_send,
        row_recv,
        row_own,
        row_out,
        row_in,
        (row_ss, row_rs, hop_ss, hop_rs),
    )
    first_all.wait_recv()
    middle = attended + first_recv[...].astype(F32).reshape(length, columns)
    mid_s[...] = middle
    high, low = split2(middle * middle)
    ones = jnp.ones((8, columns), BF)
    squares = (dot_nt(ones, high) + dot_nt(ones, low))[0:1, :]
    for j in range(n_tp):
        square_send[j] = squares
    square_all = to_tp(square_send, square_recv, square_ss, square_rs)

    own_lanes = pl.ds(pl.multiple_of(tp * columns, columns), columns)
    group = (middle * feed_gain[:, own_lanes]).astype(BF)
    slot_send[...] = dot(select_s[...], group).astype(BF).reshape(n_sp, slots, columns)

    def send_slots(i, carry):
        peer = lax.rem(sp + i, n_sp)
        remote(
            slot_send.at[peer],
            rows_s.at[y, core, sp],
            slot_ss,
            slot_rs.at[sp],
            (peer, tp),
        ).start()
        return carry

    lax.fori_loop(1, n_sp, send_slots, 0)
    pending.append(
        remote(
            slot_send.at[most], rows_s.at[0, 0, most], slot_ss, slot_rs.at[0], mate
        ).wait_send
    )
    rows_s[y, core, sp] = slot_send[sp]

    n_part = n_sp // pieces

    def ring_copy(d, step, p):
        yy = lax.rem(y + n_y + (1 - 2 * d) * (1 - step), n_y)
        to = lax.rem(y + n_y + 1 - 2 * d, n_y)
        part = rows_s.at[yy, core, pl.ds(p * n_part, n_part)]
        return remote(
            part, part, ring_ss.at[d, step, p], ring_rs.at[d, step, p], (sp, 2 * to + core)
        )

    def mate_copy(yy, c, p):
        part = rows_s.at[yy, c, pl.ds(p * n_part, n_part)]
        return remote(part, part, mate_ss.at[yy, p], mate_rs.at[yy, p], mate)

    def ahead(p):
        return p // (pieces // 2)

    for p in range(pieces):

        def wait_slots(b, carry):
            @pl.when(b != sp)
            def _():
                remote(
                    slot_send.at[b], rows_s.at[y, core, b], slot_ss, slot_rs.at[b], mate
                ).wait_recv()

            return carry

        lax.fori_loop(p * n_part, (p + 1) * n_part, wait_slots, 0)
        for d in range(2):
            if half_ring > 1 or d == ahead(p):
                ring_copy(d, 1, p).start()
        mate_copy(y, core, p).start()

    def pass_on(step):
        for p in range(pieces):
            for d in range(2):

                def one():
                    yy = lax.rem(y + n_y - (1 - 2 * d) * step, n_y)
                    ring_copy(d, step, p).wait_recv()
                    if d == ahead(p):
                        more = step < half_ring
                    else:
                        more = step + 1 < half_ring

                    @pl.when(more)
                    def _():
                        ring_copy(d, step + 1, p).start()

                    mate_copy(yy, core, p).start()

                if d == ahead(p):
                    one()
                else:
                    pl.when(step < half_ring)(one)

    for step in range(1, half_ring + 1):
        for d in range(2):
            for p in range(pieces):
                if step < half_ring or d == ahead(p):
                    pending.append(ring_copy(d, step, p).wait_send)
    for i in range(n_y):
        for p in range(pieces):
            pending.append(mate_copy(i, core, p).wait_send)
    square_all.wait_recv()
    scale = lax.rsqrt(jnp.sum(square_recv[...], axis=0) / width + EPSILON)
    high, low = split2(jnp.broadcast_to(scale, (BLK, length)).T)
    packed = jnp.where(
        iota((length, BLK), 1) < BLK // 2, high.astype(F32), low.astype(F32)
    ).astype(BF)
    scale_send[...] = dot(select_s[...], packed).astype(BF).reshape(n_sp, slots, BLK)
    scale_all = to_sp(scale_send, scale_recv, scale_ss, scale_rs)
    for load in loads[1:]:
        load.wait()
    gate_acc[...] = jnp.zeros(gate_acc.shape, F32)
    up_acc[...] = jnp.zeros(up_acc.shape, F32)

    def widen(m, carry):
        step = lax.div(m + 1, 2) + 1

        @pl.when(((m == 0) | (lax.rem(m, 2) == 1)) & (step <= half_ring))
        def _():
            pass_on(step)

        offset = jnp.where(lax.rem(m, 2) == 1, -lax.div(m + 1, 2), lax.div(m, 2))
        yy = lax.rem(y + n_y + offset, n_y)
        for p in range(pieces):
            mate_copy(yy, other, p).wait_recv()
        x = jnp.concatenate(
            [rows_s[yy, 0].reshape(count, columns), rows_s[yy, 1].reshape(count, columns)],
            axis=1,
        )
        depth = pl.ds(pl.multiple_of(yy * 2 * columns, 2 * columns), 2 * columns)
        gate_acc[...] += dot_nt(x, gate_s[:, depth])
        up_acc[...] += dot_nt(x, up_s[:, depth])
        return carry

    lax.fori_loop(0, n_y, widen, 0)
    scale_all.wait_recv()
    packed = scale_recv[...].reshape(count, BLK).astype(F32)
    scale = packed[:, 0:1] + packed[:, BLK // 2 : BLK // 2 + 1]
    gated = gate_acc[...] * scale
    hidden = gated / (1.0 + jnp.exp(-gated)) * (up_acc[...] * scale)
    hidden_s[:, 0:piece] = hidden.astype(BF)

    expert_rows = summed_product(
        hidden_s,
        down_s,
        half_send,
        half_recv,
        half_own,
        sum_out,
        sum_in,
        (half_ss, half_rs, sum_ss, sum_rs),
    )
    back_send[...] = expert_rows.astype(BF).reshape(n_sp, slots, columns)
    to_sp(back_send, back_recv, back_ss, back_rs).wait_recv()
    returned = back_recv[...].reshape(count, columns)
    routed = dot(weight_high[...], returned) + dot(weight_low[...], returned)
    result = (mid_s[...] + routed).astype(BF)
    last_send[...] = result.reshape(n_tp, rows, columns)
    to_tp(last_send, last_recv, last_ss, last_rs).wait_recv()
    for j in range(n_tp):
        out[:, j * columns : (j + 1) * columns] = last_recv[j]

    for finish in pending:
        finish()


def layer(
    n_sp,
    n_tp,
    stream_in,
    queries,
    key_rows,
    values,
    decay_low,
    decay_matrix,
    decay_bias,
    decay_shift,
    head_gain,
    output_matrix,
    feed_gain,
    routes,
    route_weights,
    expert_gate,
    specialist_widen,
    expert_down,
):
    rows, width = stream_in.shape
    length = queries.shape[0]
    hk, hv = queries.shape[1], values.shape[1]
    piece = expert_down.shape[1]
    n_y = n_tp // 2
    half_ring = n_y // 2
    slots = 2 * length // n_sp
    count = n_sp * slots
    columns = width // n_tp
    pieces = min(PIECES, n_sp)
    own = hk // n_sp
    padded = (piece + 127) // 128 * 128
    vmem, any_space = (
        pl.BlockSpec(memory_space=pltpu.VMEM),
        pl.BlockSpec(memory_space=pl.ANY),
    )
    dma = pltpu.SemaphoreType.DMA
    scratch = [
        pltpu.VMEM((hv, width), BF),
        pltpu.VMEM((piece, width), BF),
        pltpu.VMEM((piece, width), BF),
        pltpu.VMEM((padded, width), BF),
        pltpu.VMEM((length, hk), F32),
        pltpu.VMEM((length, hv), F32),
        pltpu.VMEM((2, hk, hv), F32),
        pltpu.VMEM((n_sp, own, hv + BLK), BF),
        pltpu.VMEM((n_sp, own, hv + BLK), BF),
        pltpu.VMEM((n_sp, own, hv), BF),
        pltpu.VMEM((n_sp, own, hv), BF),
        pltpu.VMEM((count, length), BF),
        pltpu.VMEM((length, count), BF),
        pltpu.VMEM((length, count), BF),
        pltpu.VMEM((length, hv), BF),
        pltpu.VMEM((n_tp, rows, columns), BF),
        pltpu.VMEM((n_tp, rows, columns), BF),
        pltpu.VMEM((n_y, pieces, length // pieces, columns), BF),
        pltpu.VMEM((n_y, pieces, length // pieces, columns), BF),
        pltpu.VMEM((n_y, pieces, length // pieces, columns), F32),
        pltpu.VMEM((2, half_ring, pieces, length // pieces, columns), BF),
        pltpu.VMEM((2, half_ring, pieces, length // pieces, columns), BF),
        pltpu.VMEM((length, columns), F32),
        pltpu.VMEM((n_tp, 1, length), F32),
        pltpu.VMEM((n_tp, 1, length), F32),
        pltpu.VMEM((n_sp, slots, BLK), BF),
        pltpu.VMEM((n_sp, slots, BLK), BF),
        pltpu.VMEM((n_sp, slots, columns), BF),
        pltpu.VMEM((n_y, 2, n_sp, slots, columns), BF),
        pltpu.VMEM((count, piece), F32),
        pltpu.VMEM((count, piece), F32),
        pltpu.VMEM((count, padded), BF),
        pltpu.VMEM((n_y, pieces, count // pieces, columns), BF),
        pltpu.VMEM((n_y, pieces, count // pieces, columns), BF),
        pltpu.VMEM((n_y, pieces, count // pieces, columns), F32),
        pltpu.VMEM((2, half_ring, pieces, count // pieces, columns), BF),
        pltpu.VMEM((2, half_ring, pieces, count // pieces, columns), BF),
        pltpu.VMEM((n_sp, slots, columns), BF),
        pltpu.VMEM((n_sp, slots, columns), BF),
        pltpu.VMEM((n_tp, rows, columns), BF),
        pltpu.VMEM((n_tp, rows, columns), BF),
        dma((4,)),
        dma,
        dma((n_sp,)),
        dma,
        dma,
        dma,
        dma,
        dma((n_y,)),
        dma((n_y,)),
        dma((2, half_ring, pieces)),
        dma((2, half_ring, pieces)),
        dma,
        dma,
        dma,
        dma,
        dma,
        dma((n_sp,)),
        dma((2, half_ring + 2, pieces)),
        dma((2, half_ring + 2, pieces)),
        dma((n_y, pieces)),
        dma((n_y, pieces)),
        dma((n_y,)),
        dma((n_y,)),
        dma((2, half_ring, pieces)),
        dma((2, half_ring, pieces)),
        dma,
        dma,
        dma,
        dma,
    ]
    return pl.pallas_call(
        functools.partial(layer_kernel, (n_sp, n_tp, rows, width, piece)),
        out_shape=jax.ShapeDtypeStruct((rows, width), BF),
        in_specs=[vmem] * 9 + [any_space] + [vmem] * 3 + [any_space] * 3,
        out_specs=vmem,
        scratch_shapes=scratch,
        compiler_params=pltpu.CompilerParams(
            collective_id=0, has_side_effects=True, vmem_limit_bytes=60 * 1024 * 1024
        ),
        name="layer",
    )(
        stream_in,
        queries,
        key_rows,
        values,
        decay_low.T,
        decay_matrix,
        decay_bias.reshape(1, -1),
        decay_shift.T,
        head_gain.reshape(1, -1),
        output_matrix,
        feed_gain.reshape(1, -1),
        routes.T,
        route_weights.T,
        jnp.swapaxes(expert_gate, 1, 2),
        jnp.swapaxes(specialist_widen, 1, 2),
        expert_down,
    )


def solution(mesh):
    in_specs = (
        P(("sp", "tp"), None),
        P("sp", "tp"),
        P("sp", "tp"),
        P("sp", "tp"),
        P("sp", None),
        P(None, "tp"),
        P("tp"),
        P("sp", "tp"),
        P(),
        P("tp", None),
        P(),
        P("sp", None),
        P("sp", None),
        P("sp", None, "tp"),
        P("sp", None, "tp"),
        P("sp", "tp", None),
    )
    return jax.shard_map(
        functools.partial(layer, mesh.shape["sp"], mesh.shape["tp"]),
        mesh=mesh,
        in_specs=in_specs,
        out_specs=P(("sp", "tp"), None),
        check_vma=False,
    )
```
